32 devices in a mesh: grp: 2 (over x), ep: 4 (over z), tp: 4 (over y, core).
Axes of the slice: x: 2, y: 2, z: 4, core: 2. Of those that a mesh axis runs over, the one named last changes fastest.
Arguments:
- token_rows: bfloat16 [4096, 2048], P(('grp', 'ep', 'tp')), parts along dimension 0, may hold values from -6 to 6
- norm_gain: float32 [2048], replicated, may hold values from 0.1 to 1.9
- norm_bias: float32 [2048], replicated, may hold values from -3 to 3
- expert_ids: int32 [4096, 2], P(('grp', 'ep', 'tp')), parts along dimension 0, may hold values from 0 to 3, as said below
- route_gates: float32 [4096, 2], P(('grp', 'ep', 'tp')), parts along dimension 0, may hold values from 0.1 to 1
- gate_weight: bfloat16 [4, 2048, 512], P('tp'), may hold values from -0.125 to 0.125
- up_weight: bfloat16 [4, 2048, 512], P('tp'), may hold values from -0.125 to 0.125
- down_weight: bfloat16 [4, 512, 2048], P('tp'), may hold values from -0.25 to 0.25
Outputs:
- combined: bfloat16 [4096, 2048], P(('grp', 'ep', 'tp')), parts along dimension 0
The draws below stay inside these ranges and needn't reach their ends.
There are 2 independent parts, one for each index of `grp`. The reference program is written for one: setup_inputs(seed, part) draws one part's arguments, and reference() takes and returns one part's arrays. A program takes and returns all parts, laid end to end along the dimension named above; an argument that names none is the same for every part. Nothing has to cross between parts.
Inputs may be any that keep to these rules, and one draw needn't show every extreme that they name: `expert_ids`: the two experts of a token are different and lie in one group: both are among 4 * g to 4 * g + 3 for some g. In the rows of one device (aligned blocks of 128 rows) no expert is named more than 64 times, and in every such block each expert of one group is named exactly 64 times; that group is the same for all blocks of a draw.
All inputs are finite; a program needn't handle non-finite values.
Results may differ from the reference program's by a relative error of at most 0.01.
Values may be sent and summed in bfloat16 or wider, within the bound.
A program may use at most 64 MiB of HBM per device.

```python
import jax
import jax.numpy as jnp
from jax import lax

D = 2048
FF = 512
GROUP_SIZE = 4
TOK_DEV = 128
EXPERTS = 4
TOKENS = 2048
N_EP = 4
N_TP = 4


def draw_expert_ids(key, part):
    experts = N_TP
    groups = experts // GROUP_SIZE
    capacity = min(4 * TOK_DEV // experts, TOK_DEV // 2)
    group_span = 2 * capacity
    slots_all = max(groups - 1, 1) * group_span
    blocks = N_EP * N_TP
    hot_group = jax.random.randint(jax.random.fold_in(key, 7), (), 0, groups, dtype=jnp.int32)

    def one_block(block_number):
        block_key = jax.random.fold_in(key, block_number + 100)
        token_order = jax.random.permutation(jax.random.fold_in(block_key, 1), TOK_DEV).astype(jnp.int32)
        shuffled = jax.random.permutation(jax.random.fold_in(block_key, 2), slots_all).astype(jnp.int32)
        rank_list = jnp.arange(TOK_DEV, dtype=jnp.int32)
        spare_slot = shuffled[jnp.clip(rank_list - group_span, 0, slots_all - 1)]
        is_hot = rank_list < group_span
        within = jnp.where(is_hot, rank_list, spare_slot % group_span)
        other_group = spare_slot // group_span
        group_id = jnp.where(is_hot, hot_group, other_group + (other_group >= hot_group).astype(jnp.int32))
        quartet = within // GROUP_SIZE
        offset = within % GROUP_SIZE
        turn_table = jax.random.randint(jax.random.fold_in(block_key, 3), (groups,), 0, GROUP_SIZE, dtype=jnp.int32)
        group_turn = turn_table[group_id]
        lead_expert = (offset + group_turn) % GROUP_SIZE
        trail_expert = (offset + 1 + quartet % (GROUP_SIZE - 1) + group_turn) % GROUP_SIZE
        flip_bits = jax.random.randint(jax.random.fold_in(block_key, 4), (TOK_DEV,), 0, 2, dtype=jnp.int32)
        first_id = jnp.where(flip_bits == 1, trail_expert, lead_expert)
        second_id = jnp.where(flip_bits == 1, lead_expert, trail_expert)
        pair_ids = jnp.stack([group_id * GROUP_SIZE + first_id, group_id * GROUP_SIZE + second_id], axis=1)
        return jnp.zeros((TOK_DEV, 2), jnp.int32).at[token_order].set(pair_ids)
    drawn = lax.map(one_block, jnp.arange(blocks, dtype=jnp.int32))
    return drawn.reshape(blocks * TOK_DEV, 2).astype(jnp.int32)


def steps_of(own_key, dims, split, least, top_value):
    def one(dim, blocks):
        draws = jax.random.uniform(jax.random.fold_in(jax.random.fold_in(own_key, 6), dim), (blocks,), jnp.float32, least / len(split), top_value / len(split))
        return jnp.repeat(jnp.exp(draws), dims[dim] // blocks).reshape((-1,) + (1,) * (len(dims) - dim - 1))

    gain = one(*split[0])
    for cut in split[1:]:
        gain = gain * one(*cut)
    return gain


def noise(stream_key, dims, scale, most, shards=(), held_as=jnp.bfloat16):
    values = scale * jax.random.normal(stream_key, dims, jnp.float32)
    if shards:
        values = values * steps_of(stream_key, dims, shards, -0.22, 0.18)
    return jnp.clip(values, -most, most).astype(held_as)


def setup_inputs(seed: int = 0, part: int = 0) -> dict:
    key_of = jax.random.split(jax.random.key(seed), 9)
    part_splits = jax.random.split(jax.random.fold_in(key_of[8], part), 9)
    token_rows = noise(part_splits[0], (TOKENS, D), 1.0, 6.0, ((0, 16),))
    norm_gain = jnp.clip(1.0 + 0.18 * jax.random.normal(key_of[1], (D,), jnp.float32), 0.1, 1.9)
    norm_bias = noise(key_of[2], (D,), 0.5, 3.0, (), jnp.float32)
    expert_ids = draw_expert_ids(jax.random.fold_in(jax.random.fold_in(key_of[8], part), 71), part)
    route_gates = jnp.clip(0.1 + 0.9 * jax.random.uniform(part_splits[4], (TOKENS, 2), jnp.float32) ** steps_of(part_splits[4], (TOKENS, 2), ((0, 16),), -0.2, 0.2), 0.1, 1.0)
    gate_weight = noise(key_of[5], (EXPERTS, D, FF), D ** -0.5, 0.125, ((0, 4),))
    up_weight = noise(key_of[6], (EXPERTS, D, FF), D ** -0.5, 0.125, ((0, 4),))
    down_weight = noise(key_of[7], (EXPERTS, FF, D), FF ** -0.5, 0.25, ((0, 4),))
    return {"token_rows": token_rows, "norm_gain": norm_gain, "norm_bias": norm_bias, "expert_ids": expert_ids, "route_gates": route_gates, "gate_weight": gate_weight, "up_weight": up_weight, "down_weight": down_weight}


EPSILON = 1e-05

def layer_norm(token_rows, gain_vec, bias_vec):
    as_float = token_rows.astype(jnp.float32)
    center = lax.optimization_barrier(jnp.mean(as_float, axis=-1, keepdims=True))
    centered = as_float - center
    variance = lax.optimization_barrier(jnp.mean(centered * centered, axis=-1, keepdims=True))
    return (centered * lax.rsqrt(variance + EPSILON) * gain_vec + bias_vec).astype(jnp.bfloat16)

def reference(token_rows, norm_gain, norm_bias, expert_ids, route_gates, gate_weight, up_weight, down_weight):
    token_count, row_width = token_rows.shape
    experts = gate_weight.shape[0]
    blocks = token_count // TOK_DEV
    capacity = min(4 * TOK_DEV // experts, TOK_DEV // 2)
    normed = layer_norm(token_rows, norm_gain, norm_bias)
    padded = jnp.concatenate([normed, jnp.zeros((1, row_width), jnp.bfloat16)], axis=0)
    block_ids = expert_ids.reshape(blocks, 2 * TOK_DEV)
    onehot = (block_ids[:, :, None] == jnp.arange(experts, dtype=jnp.int32)[None, None, :]).astype(jnp.int32)
    slot_index = lax.optimization_barrier(jnp.sum((jnp.cumsum(onehot, axis=1) - 1) * onehot, axis=2))
    block_number = jnp.arange(blocks, dtype=jnp.int32)[:, None]
    target = ((block_ids * blocks + block_number) * capacity + slot_index).reshape(-1)
    owner_row = jnp.arange(2 * token_count, dtype=jnp.int32) // 2
    row_table = jnp.full((experts * blocks * capacity,), token_count, jnp.int32).at[target].set(owner_row)
    gate_table = jnp.zeros((experts * blocks * capacity,), jnp.float32).at[target].set(route_gates.reshape(-1))
    row_table = row_table.reshape(experts, blocks * capacity)
    gate_table = gate_table.reshape(experts, blocks * capacity)

    def one_expert(summed, pieces):
        row_index, gate_matrix, up_matrix, down_matrix, row_gates = pieces
        chosen = padded[row_index]
        gate_act = jnp.dot(chosen, gate_matrix, preferred_element_type=jnp.float32)
        up_act = jnp.dot(chosen, up_matrix, preferred_element_type=jnp.float32)
        hidden = (jax.nn.silu(gate_act) * up_act).astype(jnp.bfloat16)
        output = jnp.dot(hidden, down_matrix, preferred_element_type=jnp.float32)
        weighted = (row_gates[:, None] * output).astype(jnp.bfloat16)
        summed = summed.at[row_index].add(weighted.astype(jnp.float32))
        return (summed, None)
    start = jnp.zeros((token_count + 1, row_width), jnp.float32)
    summed, _ = lax.scan(one_expert, start, (row_table, gate_weight, up_weight, down_weight, gate_table))
    return summed[:token_count].astype(jnp.bfloat16)
```

```python
import functools

import jax
import jax.numpy as jnp
from jax import lax
from jax.experimental import pallas as pl
from jax.experimental.pallas import tpu as pltpu
from jax.sharding import PartitionSpec as P

EPSILON = 1e-05
F32 = jnp.float32
BF16 = jnp.bfloat16
MESH = pl.DeviceIdType.MESH
CHUNK_ROWS = 32
NORM_ROWS = 16
BLOCKS = 1
VMEM_BYTES = 48 * 1024 * 1024
IN_SPACE = pltpu.HBM
KEEP = 8
STEP_ROWS = 32
OUT_COLS = 512


def dot(a, b):
    return jnp.dot(a, b, preferred_element_type=F32)


def kernel(
    tp_count, cores, capacity, chunks,
    tokens_hbm, gain_hbm, bias_hbm, ids_hbm, gates_hbm, wg_hbm, wu_hbm, wd_hbm,
    out_ref,
    tokens, gain_ref, bias_ref, ids_ref, gates_ref, wg, wu, wd, normed,
    near_out, near_in, near_res, near_back, far_out, far_in, far_res, far_back, total,
    w_sem, near_send, near_recv, near_rsend, near_rrecv, far_send, far_recv, far_rsend, far_rrecv,
):
    tok_count, width = tokens.shape
    chips = tp_count // cores
    far = tp_count - cores
    rows = capacity // chunks
    block = width // BLOCKS
    me = lax.axis_index("tp")
    my_chip, my_core = me // cores, me % cores

    def peer(slot):
        return (my_chip + slot // cores) % chips * cores + (my_core + slot % cores) % cores

    def origin(slot):
        return (my_chip + chips - slot // cores) % chips * cores + (my_core + cores - slot % cores) % cores

    barrier = pltpu.get_barrier_semaphore()
    for slot in range(1, tp_count):
        pl.semaphore_signal(barrier, inc=1, device_id={"tp": peer(slot)}, device_id_type=MESH)
    pairs = (
        (ids_hbm, ids_ref), (tokens_hbm, tokens), (gates_hbm, gates_ref), (gain_hbm, gain_ref), (bias_hbm, bias_ref),
        (wg_hbm.at[0], wg), (wu_hbm.at[0], wu), (wd_hbm.at[0], wd),
    )
    loads = [pltpu.make_async_copy(src, dst, w_sem.at[i]) for i, (src, dst) in enumerate(pairs)]
    for load in loads:
        load.start()

    lanes = 128 * pl.cdiv(tp_count, 128)
    t_row = lax.broadcasted_iota(jnp.int32, (tok_count, tok_count), 0)
    t_col = lax.broadcasted_iota(jnp.int32, (tok_count, tok_count), 1)
    before = jnp.where(t_row < t_col, 1.0, 0.0).astype(BF16)
    expert_of_row = lax.broadcasted_iota(jnp.int32, (lanes, tok_count), 0)
    loads[0].wait()
    ids = ids_ref[...]
    first = ids[0:1, :] == expert_of_row
    second = ids[1:2, :] == expert_of_row
    named = jnp.where(first | second, 1.0, 0.0)
    rank = dot(named.astype(BF16), before)
    place_t = jnp.where(named > 0.5, rank, -1.0)

    def place_row(slot):
        return jnp.sum(jnp.where(expert_of_row == peer(slot), place_t, 0.0), axis=0, keepdims=True).astype(jnp.int32)

    def pick(slot, start, count):
        want = start + lax.broadcasted_iota(jnp.int32, (count, tok_count), 0)
        return jnp.where(place_row(slot) == want, 1.0, 0.0).astype(BF16)

    def far_copy(c, f):
        return pltpu.make_async_remote_copy(
            far_out.at[c, f], far_in.at[c, f], far_send.at[c, f], far_recv.at[c, f],
            device_id={"tp": peer(cores + f)}, device_id_type=MESH)

    def far_return(c, f, j):
        at = pl.ds(j * block, block)
        return pltpu.make_async_remote_copy(
            far_res.at[c, f, :, at], far_back.at[c, f, :, at], far_rsend.at[c, f, j], far_rrecv.at[c, f, j],
            device_id={"tp": origin(cores + f)}, device_id_type=MESH)

    def near_copy(s):
        return pltpu.make_async_remote_copy(
            near_out.at[s], near_in.at[s], near_send.at[s], near_recv.at[s],
            device_id={"tp": peer(s)}, device_id_type=MESH)

    def near_return(s):
        return pltpu.make_async_remote_copy(
            near_res.at[s], near_back.at[s], near_rsend.at[s], near_rrecv.at[s],
            device_id={"tp": origin(s)}, device_id_type=MESH)

    for c in range(chunks):
        picks = jnp.concatenate([pick(cores + f, c * rows, rows) for f in range(far)], axis=0)
        if c == 0:
            loads[1].wait()
        far_out[c] = dot(picks, tokens[...]).astype(BF16).reshape(far, rows, width)
        if c == 0:
            pl.semaphore_wait(barrier, tp_count - 1)
        for f in range(far):
            far_copy(c, f).start()
    near_picks = jnp.concatenate([pick(s, 0, capacity) for s in range(cores)], axis=0)
    packed = dot(near_picks, tokens[...]).astype(BF16).reshape(cores, capacity, width)
    near_in[0] = packed[0]
    for s in range(1, cores):
        near_out[s] = packed[s]
        near_copy(s).start()

    for load in loads[2:5]:
        load.wait()
    gates = gates_ref[...]
    place = place_t.T
    gate_of = (jnp.where(first, gates[0:1, :], 0.0) + jnp.where(second, gates[1:2, :], 0.0)).T
    lane = lax.broadcasted_iota(jnp.int32, (tok_count, lanes), 1)

    def norm(load_rows, count):
        gain = gain_ref[...]
        bias = bias_ref[...]

        def norm_block(i, carry):
            at = pl.multiple_of(i * NORM_ROWS, NORM_ROWS)
            x = load_rows(at).astype(F32)
            center = jnp.mean(x, axis=-1, keepdims=True)
            centered = x - center
            variance = jnp.mean(centered * centered, axis=-1, keepdims=True)
            normed[pl.ds(at, NORM_ROWS), :] = (centered * lax.rsqrt(variance + EPSILON) * gain + bias).astype(BF16)
            return carry

        lax.fori_loop(0, count // NORM_ROWS, norm_block, 0)

    def hidden_of(count):
        rows_in = normed[pl.ds(0, count), :]
        gate_act = dot(rows_in, wg[...])
        up_act = dot(rows_in, wu[...])
        return (gate_act / (1.0 + jnp.exp(-gate_act)) * up_act).astype(BF16)

    for s in range(1, cores):
        near_copy(s).wait_recv()
    norm(lambda at: near_in[at // capacity, pl.ds(pl.multiple_of(at % capacity, NORM_ROWS), NORM_ROWS), :], cores * capacity)
    for load in loads[5:]:
        load.wait()
    results = dot(hidden_of(cores * capacity), wd[...]).astype(BF16).reshape(cores, capacity, width)
    near_back[0] = results[0]
    for s in range(1, cores):
        near_res[s] = results[s]
        near_return(s).start()

    def far_step(c, carry):
        for f in range(far):
            far_copy(c, f).wait_recv()
        norm(lambda at: far_in[c, at // rows, pl.ds(pl.multiple_of(at % rows, NORM_ROWS), NORM_ROWS), :], far * rows)
        hidden = hidden_of(far * rows)
        for j in range(BLOCKS):
            at = pl.ds(j * block, block)
            far_res[c, :, :, at] = dot(hidden, wd[:, at]).astype(BF16).reshape(far, rows, block)
            for f in range(far):
                far_return(c, f, j).start()
        return carry

    lax.fori_loop(0, chunks, far_step, 0)

    def spread(slots, start, count):
        want = lax.broadcasted_iota(jnp.int32, (tok_count, len(slots) * count), 1)
        high = jnp.zeros(want.shape, F32)
        for i, slot in enumerate(slots):
            mine = lane == peer(slot)
            at = jnp.sum(jnp.where(mine, place, 0.0), axis=1, keepdims=True).astype(jnp.int32) - start
            gate = jnp.sum(jnp.where(mine, gate_of, 0.0), axis=1, keepdims=True)
            at = jnp.where((at >= 0) & (at < count), at + i * count, -1)
            high = high + jnp.where(at == want, gate, 0.0)
        coarse = high.astype(BF16)
        return jnp.concatenate([coarse, (high - coarse.astype(F32)).astype(BF16)], axis=1)

    for s in range(1, cores):
        near_return(s).wait_recv()
    weights = spread(range(cores), 0, capacity)
    back = near_back[...].reshape(cores * capacity, width)
    total[...] = dot(weights, jnp.concatenate([back, back], axis=0))

    for c in range(chunks):
        weights = spread(range(cores, tp_count), c * rows, rows)
        for j in range(BLOCKS):
            at = pl.ds(j * block, block)
            for f in range(far):
                far_return(c, f, j).wait_recv()
            back = far_back[c, :, :, at].reshape(far * rows, block)
            part = total[:, at] + dot(weights, jnp.concatenate([back, back], axis=0))
            if c + 1 < chunks:
                total[:, at] = part
            else:
                out_ref[:, at] = part.astype(BF16)
    for s in range(1, cores):
        near_copy(s).wait_send()
        near_return(s).wait_send()

    def drain(c, carry):
        for f in range(far):
            far_copy(c, f).wait_send()
            for j in range(BLOCKS):
                far_return(c, f, j).wait_send()
        return carry

    lax.fori_loop(0, chunks, drain, 0)


def pair_kernel(tp_count, cores, start, sizes, opening, shared, *refs):
    refs = list(refs)
    ins = [refs.pop(0) for _ in range(8)]
    base_ref = None if opening else refs.pop(0)
    out_ref = refs.pop(0)
    flag_ref = refs.pop(0) if shared else None
    (tokens, scales, ids_all, gates_all, w_in, wd, both, total, near_back, far_out, raw, pool,
     mine, mix_out, mix_in, far_res, far_back, sem, step_recv, pass_recv, back_recv, meta_recv) = refs[:22]
    near_res, near_recv = refs[22:24] if opening else (None, None)
    flag_out, flag_in, flag_recv, here = refs[24:] if shared else [None] * 4
    tok_count, width = tokens.shape
    steps, cap = len(sizes), sum(sizes)
    starts = [sum(sizes[:k]) for k in range(steps)]
    me = lax.axis_index("tp")
    my_chip, my_core = me // cores, me % cores
    partner = my_chip * cores + (my_core + 1) % cores
    far = (my_chip + 1) % 2 * cores + my_core
    cross = (my_chip + 1) % 2 * cores + (my_core + 1) % cores
    peers = (me, partner, far, cross)
    groups, group = 1, 0
    if shared:
        outer, inner = lax.axis_size("ep"), lax.axis_size("grp")
        groups = outer * inner
        group = lax.axis_index("ep") * inner + lax.axis_index("grp")

    def member(k):
        other = (group + k) % groups
        return other, {"ep": other // inner, "grp": other % inner}

    barrier = pltpu.get_barrier_semaphore()
    for slot in range(1, tp_count):
        pl.semaphore_signal(barrier, inc=1, device_id={"tp": peers[slot]}, device_id_type=MESH)
    for k in range(1, groups):
        other, where = member(k)

        @pl.when(other > group)
        def _(where=where):
            pl.semaphore_signal(barrier, inc=1, device_id=where, device_id_type=MESH)

    moves = [
        (ins[3], ids_all.at[0], 0), (ins[0], tokens, 1), (ins[4], gates_all.at[0], 2),
        (ins[1], scales.at[0], 3), (ins[2], scales.at[1], 3),
        (ins[5].at[0], w_in.at[0], 4), (ins[6].at[0], w_in.at[1], 4), (ins[7].at[0], wd, 5),
    ]
    for src, dst, i in moves:
        pltpu.make_async_copy(src, dst, sem.at[i]).start()

    def landed(ref, i):
        pltpu.make_async_copy(ref, ref, sem.at[i]).wait()

    def copy(src, dst, send, recv, tp):
        return pltpu.make_async_remote_copy(src, dst, sem.at[send], recv, device_id={"tp": tp}, device_id_type=MESH)

    def span(k):
        return pl.ds(starts[k], sizes[k])

    def far_copy(k):
        dst = raw if k == 0 and opening else pool.at[pl.ds(2 * starts[k], sizes[k])]
        return copy(far_out.at[span(k)], dst, 0, step_recv.at[k], far)

    def relay(k):
        src = pool.at[pl.ds(2 * starts[k], sizes[k])]
        return copy(src, pool.at[pl.ds(2 * starts[k] + sizes[k], sizes[k])], 4, pass_recv.at[0, k % 2], partner)

    def mix(k):
        return copy(mix_out.at[span(k)], mix_in.at[span(k)], 5, pass_recv.at[1, k % 2], partner)

    def far_return(k):
        return copy(far_res.at[span(k)], far_back.at[span(k)], 6, back_recv.at[(k + 1) // steps], far)

    def meta(i, slot):
        table = (ids_all, gates_all)[i]
        return copy(table.at[0], table.at[slot], 1 + i, meta_recv.at[i], peers[slot])

    def near_copy():
        return copy(both.at[pl.ds(0, tok_count)], both.at[pl.ds(tok_count, tok_count)], 3, near_recv.at[0], partner)

    def near_return():
        return copy(near_res, near_back, 3, near_recv.at[1], partner)

    def flag_copy(k):
        return pltpu.make_async_remote_copy(
            flag_out, flag_in.at[k], sem.at[7], flag_recv.at[0], device_id=member(k)[1], device_id_type=MESH)

    def sent(ref, i):
        pltpu.make_async_remote_copy(ref, ref, sem.at[i], sem.at[i], device_id={"tp": far}, device_id_type=MESH).wait_send()

    def received(ref, recv):
        pltpu.make_async_remote_copy(ref, ref, sem.at[0], recv, device_id={"tp": far}, device_id_type=MESH).wait_recv()

    row = lax.broadcasted_iota(jnp.int32, (tok_count, tok_count), 0)
    col = lax.broadcasted_iota(jnp.int32, (tok_count, tok_count), 1)
    before = jnp.where(row < col, 1.0, 0.0).astype(BF16)

    def leaves(slot):
        low = peers[slot] // cores * cores
        ids = ids_all[slot]
        away = (ids < low) | (ids >= low + cores)
        return jnp.where(away[0:1, :] | away[1:2, :], 1.0, 0.0)

    def place_of(leaving):
        rank = dot(jnp.broadcast_to(leaving, (16, tok_count)).astype(BF16), before)[0:1, :]
        return jnp.where(leaving > 0.5, rank, -1.0)

    def pick(place, k):
        want = start + starts[k] + lax.broadcasted_iota(jnp.int32, (sizes[k], tok_count), 0)
        return place.astype(jnp.int32) == want

    def gate_row(slot):
        mine_of = jnp.where(ids_all[slot] == me, gates_all[slot], 0.0)
        return mine_of[0:1, :] + mine_of[1:2, :]

    def column(chosen, values):
        return jnp.sum(jnp.where(chosen, values, 0.0), axis=1, keepdims=True)

    def pack(k, rows):
        chosen = jnp.where(pick(place, k), 1.0, 0.0).astype(BF16)
        far_out[span(k), :] = dot(chosen, rows).astype(BF16)

    def norm(src, dst, count):
        gain, bias = scales[0], scales[1]

        def norm_block(i, carry):
            at = pl.ds(pl.multiple_of(i * NORM_ROWS, NORM_ROWS), NORM_ROWS)
            x = src[at, :].astype(F32)
            center = jnp.mean(x, axis=-1, keepdims=True)
            centered = x - center
            variance = jnp.mean(centered * centered, axis=-1, keepdims=True)
            dst[at, :] = (centered * lax.rsqrt(variance + EPSILON) * gain + bias).astype(BF16)
            return carry

        lax.fori_loop(0, count // NORM_ROWS, norm_block, 0)

    def hidden_of(rows_in):
        gate_act = dot(rows_in, w_in[0])
        up_act = dot(rows_in, w_in[1])
        return (gate_act / (1.0 + jnp.exp(-gate_act)) * up_act).astype(BF16)

    blocks = [pl.ds(i, min(OUT_COLS, width - i)) for i in range(0, width, OUT_COLS)]
    own_rows = both.at[pl.ds(0, tok_count)]

    landed(ids_all.at[0], 0)
    leaving = leaves(0)
    place = place_of(leaving)
    landed(tokens, 1)
    if opening:
        pack(0, tokens[...])
    else:
        landed(scales, 3)
        norm(tokens, own_rows, tok_count)
        pack(0, own_rows[...])
    landed(gates_all.at[0], 2)
    pl.semaphore_wait(barrier, tp_count - 1 + group)
    for slot in range(tp_count - 1, 0, -1):
        for i in range(2):
            meta(i, slot).start()
    far_copy(0).start()
    for k in range(1, groups):
        other, where = member(k)

        @pl.when(other < group)
        def _(where=where):
            pl.semaphore_signal(here, inc=1, device_id=where, device_id_type=MESH)

    if opening:
        landed(scales, 3)
        norm(tokens, own_rows, tok_count)
    for k in range(1, steps):
        pack(k, own_rows[...])
        far_copy(k).start()
    if opening:
        near_copy().start()

    for i in range(2):
        received((ids_all, gates_all)[i].at[pl.ds(1, tp_count - 1)], meta_recv.at[i])
    far_leaving, cross_leaving = leaves(2), leaves(3)
    far_place, far_gate = place_of(far_leaving), gate_row(2)
    cross_place, cross_gate = place_of(cross_leaving), gate_row(3)
    if shared:
        count = jnp.sum(leaving, axis=1, keepdims=True)
        for other in (leaves(1), far_leaving, cross_leaving):
            count = jnp.maximum(count, jnp.sum(other, axis=1, keepdims=True))
        flag_out[...] = jnp.broadcast_to(jnp.where(count > cap, 1.0, 0.0), flag_out.shape)
    landed(w_in, 4)
    landed(wd, 5)
    if opening:
        gate_own = column(row == col, gate_row(0))
        gate_near = column(row == col, gate_row(1))
        near_copy().wait_recv()
        hidden = hidden_of(both[...])
        for cols in blocks:
            result = dot(hidden, wd[:, cols])
            total[:, cols] = result[:tok_count] * gate_own
            near_res[:, cols] = (result[tok_count:] * gate_near).astype(BF16)
        near_return().start()

    far_copy(0).wait_recv()
    if opening:
        norm(raw, pool, sizes[0])
    relay(0).start()
    for k in range(steps):
        gate_far = column(pick(far_place, k), far_gate)
        gate_cross = column(pick(cross_place, k), cross_gate)
        relay(k).wait_recv()
        hidden = hidden_of(pool[pl.ds(2 * starts[k], 2 * sizes[k]), :])
        for cols in blocks:
            result = dot(hidden, wd[:, cols])
            mine[pl.ds(0, sizes[k]), cols] = result[:sizes[k]] * gate_far
            mix_out[span(k), cols] = (result[sizes[k]:] * gate_cross).astype(BF16)
        mix(k).start()
        if k + 1 < steps:
            far_copy(k + 1).wait_recv()
            relay(k + 1).start()
        mix(k).wait_recv()
        far_res[span(k), :] = (mine[pl.ds(0, sizes[k]), :] + mix_in[span(k), :].astype(F32)).astype(BF16)
        far_return(k).start()
        if shared and k == 0:
            @pl.when(group < groups - 1)
            def _():
                pl.semaphore_wait(here, groups - 1 - group)

            for other in range(1, groups):
                flag_copy(other).start()

    place_col = column(row == col, place).astype(jnp.int32)

    def spread(at, count):
        want = start + at + lax.broadcasted_iota(jnp.int32, (tok_count, count), 1)
        return dot(jnp.where(place_col == want, 1.0, 0.0).astype(BF16), far_back[pl.ds(at, count), :])

    if opening:
        near_return().wait_recv()
        total[...] = total[...] + near_back[...].astype(F32)
    else:
        total[...] = base_ref[...].astype(F32)
    if shared:
        received(flag_in.at[pl.ds(1, groups - 1)], flag_recv.at[0])
        flag = flag_out[...]
        for k in range(1, groups):
            flag = jnp.maximum(flag, flag_in[k])
        flag_ref[0, 0] = jnp.max(flag).astype(jnp.int32)
    if steps > 1:
        received(far_back.at[pl.ds(0, starts[-1])], back_recv.at[0])
        total[...] = total[...] + spread(0, starts[-1])
    far_return(steps - 1).wait_recv()
    out_ref[...] = (total[...] + spread(starts[-1], sizes[-1])).astype(BF16)

    for i in (0, 4, 5, 6):
        sent(far_out, i)
    for i in range(2):
        sent((ids_all, gates_all)[i].at[pl.ds(1, tp_count - 1)], 1 + i)
    if opening:
        sent(both, 3)
    if shared:
        sent(flag_in.at[pl.ds(1, groups - 1)], 7)


def pair_call(tp_count, cores, start, sizes, shared, arrays, base=None):
    tok_count, width = arrays[0].shape
    hidden = arrays[5].shape[2]
    opening = base is None
    cap = sum(sizes)
    groups = lax.axis_size("ep") * lax.axis_size("grp")
    whole = pltpu.VMEM((tok_count, width), BF16)
    part = pltpu.VMEM((cap, width), BF16)
    dma = pltpu.SemaphoreType.DMA
    scratch = [
        whole,
        pltpu.VMEM((2, 1, width), F32),
        pltpu.VMEM((tp_count, 2, tok_count), jnp.int32),
        pltpu.VMEM((tp_count, 2, tok_count), F32),
        pltpu.VMEM((2, width, hidden), BF16),
        pltpu.VMEM((hidden, width), BF16),
        pltpu.VMEM((2 * tok_count, width), BF16),
        pltpu.VMEM((tok_count, width), F32),
        whole,
        part,
        pltpu.VMEM((sizes[0], width), BF16),
        pltpu.VMEM((2 * cap, width), BF16),
        pltpu.VMEM((max(sizes), width), F32),
        part, part, part, part,
        dma((8,)), dma((len(sizes),)), dma((2, 2)), dma((2,)), dma((2,)),
    ]
    if opening:
        scratch += [whole, dma((2,))]
    if shared:
        scratch += [
            pltpu.VMEM((8, 128), F32), pltpu.VMEM((groups, 8, 128), F32), dma((1,)), pltpu.SemaphoreType.REGULAR,
        ]
    out_shape = [pltpu.VMEM((tok_count, width), BF16)]
    out_specs = [pl.BlockSpec(memory_space=pltpu.VMEM)]
    if shared:
        out_shape.append(pltpu.SMEM((1, 1), jnp.int32))
        out_specs.append(pl.BlockSpec(memory_space=pltpu.SMEM))
    in_specs = [pl.BlockSpec(memory_space=IN_SPACE)] * len(arrays)
    arrays = [pltpu.with_memory_space_constraint(x, pltpu.HBM) for x in arrays]
    if not opening:
        arrays.append(base)
        in_specs.append(pl.BlockSpec(memory_space=pltpu.VMEM))
    return pl.pallas_call(
        functools.partial(pair_kernel, tp_count, cores, start, sizes, opening, shared),
        out_shape=out_shape,
        in_specs=in_specs,
        out_specs=out_specs,
        scratch_shapes=scratch,
        compiler_params=pltpu.CompilerParams(
            collective_id=0 if opening else 1, has_side_effects=True, vmem_limit_bytes=VMEM_BYTES
        ),
    )(*arrays)


def cut(rows):
    return [min(STEP_ROWS, rows - at) for at in range(0, rows, STEP_ROWS)]


def pair_shards(tp_count, cores, arrays):
    tok_count = arrays[0].shape[0]
    cap = tok_count - (tok_count // KEEP if KEEP else 0)
    if cap == tok_count:
        return pair_call(tp_count, cores, 0, cut(cap), False, arrays)[0]
    out, flag = pair_call(tp_count, cores, 0, cut(cap), True, arrays)
    return lax.cond(
        flag[0, 0] > 0,
        lambda: pair_call(tp_count, cores, cap, cut(tok_count - cap), False, arrays, out)[0],
        lambda: out,
    )


def shards(token_rows, norm_gain, norm_bias, expert_ids, route_gates, gate_weight, up_weight, down_weight):
    tok_count, width = token_rows.shape
    hidden = gate_weight.shape[2]
    tp_count = lax.axis_size("tp")
    capacity = min(4 * tok_count // tp_count, tok_count // 2)
    cores = 2
    arrays = [
        token_rows, norm_gain.reshape(1, width), norm_bias.reshape(1, width),
        expert_ids.T, route_gates.T, gate_weight, up_weight, down_weight,
    ]
    if tp_count == 2 * cores:
        return pair_shards(tp_count, cores, arrays)
    far = tp_count - cores
    chunks = max(1, capacity // CHUNK_ROWS)
    rows = capacity // chunks
    near = pltpu.VMEM((cores, capacity, width), BF16)
    distant = pltpu.VMEM((chunks, far, rows, width), BF16)
    near_sem = pltpu.SemaphoreType.DMA((cores,))
    far_sem = pltpu.SemaphoreType.DMA((chunks, far))
    ret_sem = pltpu.SemaphoreType.DMA((chunks, far, BLOCKS))
    return pl.pallas_call(
        functools.partial(kernel, tp_count, cores, capacity, chunks),
        out_shape=pltpu.VMEM((tok_count, width), BF16),
        in_specs=[pl.BlockSpec(memory_space=IN_SPACE)] * 8,
        out_specs=pl.BlockSpec(memory_space=pltpu.VMEM),
        scratch_shapes=[
            pltpu.VMEM((tok_count, width), BF16),
            pltpu.VMEM((1, width), F32),
            pltpu.VMEM((1, width), F32),
            pltpu.VMEM((2, tok_count), jnp.int32),
            pltpu.VMEM((2, tok_count), F32),
            pltpu.VMEM((width, hidden), BF16),
            pltpu.VMEM((width, hidden), BF16),
            pltpu.VMEM((hidden, width), BF16),
            pltpu.VMEM((max(cores * capacity, far * rows), width), BF16),
            near, near, near, near,
            distant, distant, distant, distant,
            pltpu.VMEM((tok_count, width), F32),
            pltpu.SemaphoreType.DMA((8,)),
            near_sem, near_sem, near_sem, near_sem,
            far_sem, far_sem, ret_sem, ret_sem,
        ],
        compiler_params=pltpu.CompilerParams(
            collective_id=0, has_side_effects=True, vmem_limit_bytes=VMEM_BYTES
        ),
    )(*(pltpu.with_memory_space_constraint(x, pltpu.HBM) for x in arrays))


def solution(mesh):
    rows = P(("grp", "ep", "tp"), None)
    weight = P("tp", None, None)
    return jax.shard_map(
        shards, mesh=mesh,
        in_specs=(rows, P(), P(), rows, rows, weight, weight, weight),
        out_specs=rows, check_vma=False,
    )
```

```python
import functools

import jax
import jax.numpy as jnp
from jax import lax
from jax.experimental import pallas as pl
from jax.experimental.pallas import tpu as pltpu
from jax.sharding import PartitionSpec as P

EPSILON = 1e-05
F32 = jnp.float32
BF16 = jnp.bfloat16
MESH = pl.DeviceIdType.MESH
CHUNK_ROWS = 32
NORM_ROWS = 16
BLOCKS = 1
VMEM_BYTES = 48 * 1024 * 1024
IN_SPACE = pltpu.HBM
KEEP = 8
STEP_ROWS = 32
OUT_COLS = 512
TAIL_COLS = 1024


def dot(a, b):
    return jnp.dot(a, b, preferred_element_type=F32)


def kernel(
    tp_count, cores, capacity, chunks,
    tokens_hbm, gain_hbm, bias_hbm, ids_hbm, gates_hbm, wg_hbm, wu_hbm, wd_hbm,
    out_ref,
    tokens, gain_ref, bias_ref, ids_ref, gates_ref, wg, wu, wd, normed,
    near_out, near_in, near_res, near_back, far_out, far_in, far_res, far_back, total,
    w_sem, near_send, near_recv, near_rsend, near_rrecv, far_send, far_recv, far_rsend, far_rrecv,
):
    tok_count, width = tokens.shape
    chips = tp_count // cores
    far = tp_count - cores
    rows = capacity // chunks
    block = width // BLOCKS
    me = lax.axis_index("tp")
    my_chip, my_core = me // cores, me % cores

    def peer(slot):
        return (my_chip + slot // cores) % chips * cores + (my_core + slot % cores) % cores

    def origin(slot):
        return (my_chip + chips - slot // cores) % chips * cores + (my_core + cores - slot % cores) % cores

    barrier = pltpu.get_barrier_semaphore()
    for slot in range(1, tp_count):
        pl.semaphore_signal(barrier, inc=1, device_id={"tp": peer(slot)}, device_id_type=MESH)
    pairs = (
        (ids_hbm, ids_ref), (tokens_hbm, tokens), (gates_hbm, gates_ref), (gain_hbm, gain_ref), (bias_hbm, bias_ref),
        (wg_hbm.at[0], wg), (wu_hbm.at[0], wu), (wd_hbm.at[0], wd),
    )
    loads = [pltpu.make_async_copy(src, dst, w_sem.at[i]) for i, (src, dst) in enumerate(pairs)]
    for load in loads:
        load.start()

    lanes = 128 * pl.cdiv(tp_count, 128)
    t_row = lax.broadcasted_iota(jnp.int32, (tok_count, tok_count), 0)
    t_col = lax.broadcasted_iota(jnp.int32, (tok_count, tok_count), 1)
    before = jnp.where(t_row < t_col, 1.0, 0.0).astype(BF16)
    expert_of_row = lax.broadcasted_iota(jnp.int32, (lanes, tok_count), 0)
    loads[0].wait()
    ids = ids_ref[...]
    first = ids[0:1, :] == expert_of_row
    second = ids[1:2, :] == expert_of_row
    named = jnp.where(first | second, 1.0, 0.0)
    rank = dot(named.astype(BF16), before)
    place_t = jnp.where(named > 0.5, rank, -1.0)

    def place_row(slot):
        return jnp.sum(jnp.where(expert_of_row == peer(slot), place_t, 0.0), axis=0, keepdims=True).astype(jnp.int32)

    def pick(slot, start, count):
        want = start + lax.broadcasted_iota(jnp.int32, (count, tok_count), 0)
        return jnp.where(place_row(slot) == want, 1.0, 0.0).astype(BF16)

    def far_copy(c, f):
        return pltpu.make_async_remote_copy(
            far_out.at[c, f], far_in.at[c, f], far_send.at[c, f], far_recv.at[c, f],
            device_id={"tp": peer(cores + f)}, device_id_type=MESH)

    def far_return(c, f, j):
        at = pl.ds(j * block, block)
        return pltpu.make_async_remote_copy(
            far_res.at[c, f, :, at], far_back.at[c, f, :, at], far_rsend.at[c, f, j], far_rrecv.at[c, f, j],
            device_id={"tp": origin(cores + f)}, device_id_type=MESH)

    def near_copy(s):
        return pltpu.make_async_remote_copy(
            near_out.at[s], near_in.at[s], near_send.at[s], near_recv.at[s],
            device_id={"tp": peer(s)}, device_id_type=MESH)

    def near_return(s):
        return pltpu.make_async_remote_copy(
            near_res.at[s], near_back.at[s], near_rsend.at[s], near_rrecv.at[s],
            device_id={"tp": origin(s)}, device_id_type=MESH)

    for c in range(chunks):
        picks = jnp.concatenate([pick(cores + f, c * rows, rows) for f in range(far)], axis=0)
        if c == 0:
            loads[1].wait()
        far_out[c] = dot(picks, tokens[...]).astype(BF16).reshape(far, rows, width)
        if c == 0:
            pl.semaphore_wait(barrier, tp_count - 1)
        for f in range(far):
            far_copy(c, f).start()
    near_picks = jnp.concatenate([pick(s, 0, capacity) for s in range(cores)], axis=0)
    packed = dot(near_picks, tokens[...]).astype(BF16).reshape(cores, capacity, width)
    near_in[0] = packed[0]
    for s in range(1, cores):
        near_out[s] = packed[s]
        near_copy(s).start()

    for load in loads[2:5]:
        load.wait()
    gates = gates_ref[...]
    place = place_t.T
    gate_of = (jnp.where(first, gates[0:1, :], 0.0) + jnp.where(second, gates[1:2, :], 0.0)).T
    lane = lax.broadcasted_iota(jnp.int32, (tok_count, lanes), 1)

    def norm(load_rows, count):
        gain = gain_ref[...]
        bias = bias_ref[...]

        def norm_block(i, carry):
            at = pl.multiple_of(i * NORM_ROWS, NORM_ROWS)
            x = load_rows(at).astype(F32)
            center = jnp.mean(x, axis=-1, keepdims=True)
            centered = x - center
            variance = jnp.mean(centered * centered, axis=-1, keepdims=True)
            normed[pl.ds(at, NORM_ROWS), :] = (centered * lax.rsqrt(variance + EPSILON) * gain + bias).astype(BF16)
            return carry

        lax.fori_loop(0, count // NORM_ROWS, norm_block, 0)

    def hidden_of(count):
        rows_in = normed[pl.ds(0, count), :]
        gate_act = dot(rows_in, wg[...])
        up_act = dot(rows_in, wu[...])
        return (gate_act / (1.0 + jnp.exp(-gate_act)) * up_act).astype(BF16)

    for s in range(1, cores):
        near_copy(s).wait_recv()
    norm(lambda at: near_in[at // capacity, pl.ds(pl.multiple_of(at % capacity, NORM_ROWS), NORM_ROWS), :], cores * capacity)
    for load in loads[5:]:
        load.wait()
    results = dot(hidden_of(cores * capacity), wd[...]).astype(BF16).reshape(cores, capacity, width)
    near_back[0] = results[0]
    for s in range(1, cores):
        near_res[s] = results[s]
        near_return(s).start()

    def far_step(c, carry):
        for f in range(far):
            far_copy(c, f).wait_recv()
        norm(lambda at: far_in[c, at // rows, pl.ds(pl.multiple_of(at % rows, NORM_ROWS), NORM_ROWS), :], far * rows)
        hidden = hidden_of(far * rows)
        for j in range(BLOCKS):
            at = pl.ds(j * block, block)
            far_res[c, :, :, at] = dot(hidden, wd[:, at]).astype(BF16).reshape(far, rows, block)
            for f in range(far):
                far_return(c, f, j).start()
        return carry

    lax.fori_loop(0, chunks, far_step, 0)

    def spread(slots, start, count):
        want = lax.broadcasted_iota(jnp.int32, (tok_count, len(slots) * count), 1)
        high = jnp.zeros(want.shape, F32)
        for i, slot in enumerate(slots):
            mine = lane == peer(slot)
            at = jnp.sum(jnp.where(mine, place, 0.0), axis=1, keepdims=True).astype(jnp.int32) - start
            gate = jnp.sum(jnp.where(mine, gate_of, 0.0), axis=1, keepdims=True)
            at = jnp.where((at >= 0) & (at < count), at + i * count, -1)
            high = high + jnp.where(at == want, gate, 0.0)
        coarse = high.astype(BF16)
        return jnp.concatenate([coarse, (high - coarse.astype(F32)).astype(BF16)], axis=1)

    for s in range(1, cores):
        near_return(s).wait_recv()
    weights = spread(range(cores), 0, capacity)
    back = near_back[...].reshape(cores * capacity, width)
    total[...] = dot(weights, jnp.concatenate([back, back], axis=0))

    for c in range(chunks):
        weights = spread(range(cores, tp_count), c * rows, rows)
        for j in range(BLOCKS):
            at = pl.ds(j * block, block)
            for f in range(far):
                far_return(c, f, j).wait_recv()
            back = far_back[c, :, :, at].reshape(far * rows, block)
            part = total[:, at] + dot(weights, jnp.concatenate([back, back], axis=0))
            if c + 1 < chunks:
                total[:, at] = part
            else:
                out_ref[:, at] = part.astype(BF16)
    for s in range(1, cores):
        near_copy(s).wait_send()
        near_return(s).wait_send()

    def drain(c, carry):
        for f in range(far):
            far_copy(c, f).wait_send()
            for j in range(BLOCKS):
                far_return(c, f, j).wait_send()
        return carry

    lax.fori_loop(0, chunks, drain, 0)


def pair_kernel(tp_count, cores, start, sizes, opening, shared, *refs):
    refs = list(refs)
    ins = [refs.pop(0) for _ in range(8)]
    base_ref = None if opening else refs.pop(0)
    out_ref = refs.pop(0)
    flag_ref = refs.pop(0) if shared else None
    (tokens, scales, ids_all, gates_all, w_in, wd, both, total, near_back, far_out, raw, pool,
     mine, mix_out, mix_in, far_res, far_back, sem, step_recv, pass_recv, back_recv, meta_recv) = refs[:22]
    near_res, near_recv = refs[22:24] if opening else (None, None)
    flag_out, flag_in, flag_recv, here = refs[24:] if shared else [None] * 4
    tok_count, width = tokens.shape
    steps, cap = len(sizes), sum(sizes)
    starts = [sum(sizes[:k]) for k in range(steps)]
    me = lax.axis_index("tp")
    my_chip, my_core = me // cores, me % cores
    partner = my_chip * cores + (my_core + 1) % cores
    far = (my_chip + 1) % 2 * cores + my_core
    cross = (my_chip + 1) % 2 * cores + (my_core + 1) % cores
    peers = (me, partner, far, cross)
    groups, group = 1, 0
    if shared:
        outer, inner = lax.axis_size("ep"), lax.axis_size("grp")
        groups = outer * inner
        group = lax.axis_index("ep") * inner + lax.axis_index("grp")

    def member(k):
        other = (group + k) % groups
        return other, {"ep": other // inner, "grp": other % inner}

    barrier = pltpu.get_barrier_semaphore()
    for slot in range(1, tp_count):
        pl.semaphore_signal(barrier, inc=1, device_id={"tp": peers[slot]}, device_id_type=MESH)
    for k in range(1, groups):
        other, where = member(k)

        @pl.when(other > group)
        def _(where=where):
            pl.semaphore_signal(barrier, inc=1, device_id=where, device_id_type=MESH)

    moves = [
        (ins[3], ids_all.at[0], 0), (ins[0], tokens, 1), (ins[4], gates_all.at[0], 2),
        (ins[1], scales.at[0], 3), (ins[2], scales.at[1], 3),
        (ins[5].at[0], w_in.at[0], 4), (ins[6].at[0], w_in.at[1], 4), (ins[7].at[0], wd, 5),
    ]
    def load(some):
        for src, dst, i in some:
            pltpu.make_async_copy(src, dst, sem.at[i]).start()

    load(moves[:5])

    def landed(ref, i):
        pltpu.make_async_copy(ref, ref, sem.at[i]).wait()

    def copy(src, dst, send, recv, tp):
        return pltpu.make_async_remote_copy(src, dst, sem.at[send], recv, device_id={"tp": tp}, device_id_type=MESH)

    def span(k):
        return pl.ds(starts[k], sizes[k])

    def far_copy(k):
        dst = raw if k == 0 and opening else pool.at[pl.ds(2 * starts[k], sizes[k])]
        return copy(far_out.at[span(k)], dst, 0, step_recv.at[k], far)

    def relay(k):
        src = pool.at[pl.ds(2 * starts[k], sizes[k])]
        return copy(src, pool.at[pl.ds(2 * starts[k] + sizes[k], sizes[k])], 4, pass_recv.at[0, k % 2], partner)

    def mix(k):
        return copy(mix_out.at[span(k)], mix_in.at[span(k)], 5, pass_recv.at[1, k % 2], partner)

    def far_return(k, part=None):
        if part is None:
            return copy(far_res.at[span(k)], far_back.at[span(k)], 6, back_recv.at[0], far)
        at = (span(k), halves[part])
        return copy(far_res.at[at], far_back.at[at], 6, back_recv.at[1 + part], far)

    def meta(i, slot):
        table = (ids_all, gates_all)[i]
        return copy(table.at[0], table.at[slot], 1 + i, meta_recv.at[i], peers[slot])

    def near_copy():
        return copy(both.at[pl.ds(0, tok_count)], both.at[pl.ds(tok_count, tok_count)], 3, near_recv.at[0], partner)

    def near_return():
        return copy(near_res, near_back, 3, near_recv.at[1], partner)

    def flag_copy(k):
        return pltpu.make_async_remote_copy(
            flag_out, flag_in.at[k], sem.at[7], flag_recv.at[0], device_id=member(k)[1], device_id_type=MESH)

    def sent(ref, i):
        pltpu.make_async_remote_copy(ref, ref, sem.at[i], sem.at[i], device_id={"tp": far}, device_id_type=MESH).wait_send()

    def received(ref, recv):
        pltpu.make_async_remote_copy(ref, ref, sem.at[0], recv, device_id={"tp": far}, device_id_type=MESH).wait_recv()

    row = lax.broadcasted_iota(jnp.int32, (tok_count, tok_count), 0)
    col = lax.broadcasted_iota(jnp.int32, (tok_count, tok_count), 1)
    before = jnp.where(row < col, 1.0, 0.0).astype(BF16)

    def leaves(slot):
        low = peers[slot] // cores * cores
        ids = ids_all[slot]
        away = (ids < low) | (ids >= low + cores)
        return jnp.where(away[0:1, :] | away[1:2, :], 1.0, 0.0)

    def place_of(leaving):
        rank = dot(jnp.broadcast_to(leaving, (16, tok_count)).astype(BF16), before)[0:1, :]
        return jnp.where(leaving > 0.5, rank, -1.0)

    def pick(place, k):
        want = start + starts[k] + lax.broadcasted_iota(jnp.int32, (sizes[k], tok_count), 0)
        return place.astype(jnp.int32) == want

    def gate_row(slot):
        mine_of = jnp.where(ids_all[slot] == me, gates_all[slot], 0.0)
        return mine_of[0:1, :] + mine_of[1:2, :]

    def column(chosen, values):
        return jnp.sum(jnp.where(chosen, values, 0.0), axis=1, keepdims=True)

    def pack(k, rows):
        chosen = jnp.where(pick(place, k), 1.0, 0.0).astype(BF16)
        far_out[span(k), :] = dot(chosen, rows).astype(BF16)

    def norm(src, dst, count):
        gain, bias = scales[0], scales[1]

        def norm_block(i, carry):
            at = pl.ds(pl.multiple_of(i * NORM_ROWS, NORM_ROWS), NORM_ROWS)
            x = src[at, :].astype(F32)
            center = jnp.mean(x, axis=-1, keepdims=True)
            centered = x - center
            variance = jnp.mean(centered * centered, axis=-1, keepdims=True)
            dst[at, :] = (centered * lax.rsqrt(variance + EPSILON) * gain + bias).astype(BF16)
            return carry

        lax.fori_loop(0, count // NORM_ROWS, norm_block, 0)

    def hidden_of(rows_in):
        gate_act = dot(rows_in, w_in[0])
        up_act = dot(rows_in, w_in[1])
        return (gate_act / (1.0 + jnp.exp(-gate_act)) * up_act).astype(BF16)

    blocks = [pl.ds(i, min(OUT_COLS, width - i)) for i in range(0, width, OUT_COLS)]
    halves = [pl.ds(i, min(TAIL_COLS, width - i)) for i in range(0, width, TAIL_COLS)]
    own_rows = both.at[pl.ds(0, tok_count)]

    landed(ids_all.at[0], 0)
    leaving = leaves(0)
    place = place_of(leaving)
    landed(tokens, 1)
    load(moves[5:])
    if opening:
        pack(0, tokens[...])
    else:
        landed(scales, 3)
        norm(tokens, own_rows, tok_count)
        pack(0, own_rows[...])
    landed(gates_all.at[0], 2)
    pl.semaphore_wait(barrier, tp_count - 1 + group)
    for slot in range(tp_count - 1, 0, -1):
        for i in range(2):
            meta(i, slot).start()
    far_copy(0).start()
    for k in range(1, groups):
        other, where = member(k)

        @pl.when(other < group)
        def _(where=where):
            pl.semaphore_signal(here, inc=1, device_id=where, device_id_type=MESH)

    if opening:
        landed(scales, 3)
        norm(tokens, own_rows, tok_count)
    for k in range(1, steps):
        pack(k, own_rows[...])
        far_copy(k).start()
    if opening:
        near_copy().start()

    for i in range(2):
        received((ids_all, gates_all)[i].at[pl.ds(1, tp_count - 1)], meta_recv.at[i])
    far_leaving, cross_leaving = leaves(2), leaves(3)
    far_place, far_gate = place_of(far_leaving), gate_row(2)
    cross_place, cross_gate = place_of(cross_leaving), gate_row(3)
    if shared:
        count = jnp.sum(leaving, axis=1, keepdims=True)
        for other in (leaves(1), far_leaving, cross_leaving):
            count = jnp.maximum(count, jnp.sum(other, axis=1, keepdims=True))
        flag_out[...] = jnp.broadcast_to(jnp.where(count > cap, 1.0, 0.0), flag_out.shape)
    landed(w_in, 4)
    landed(wd, 5)
    far_copy(0).wait_recv()
    if opening:
        norm(raw, pool, sizes[0])
    relay(0).start()
    for k in range(steps):
        gate_far = column(pick(far_place, k), far_gate)
        gate_cross = column(pick(cross_place, k), cross_gate)
        relay(k).wait_recv()
        hidden = hidden_of(pool[pl.ds(2 * starts[k], 2 * sizes[k]), :])
        for cols in blocks:
            result = dot(hidden, wd[:, cols])
            mine[pl.ds(0, sizes[k]), cols] = result[:sizes[k]] * gate_far
            mix_out[span(k), cols] = (result[sizes[k]:] * gate_cross).astype(BF16)
        mix(k).start()
        if k + 1 < steps:
            far_copy(k + 1).wait_recv()
            relay(k + 1).start()
        mix(k).wait_recv()
        far_res[span(k), :] = (mine[pl.ds(0, sizes[k]), :] + mix_in[span(k), :].astype(F32)).astype(BF16)
        if k + 1 < steps:
            far_return(k).start()
        else:
            for part in range(len(halves)):
                far_return(k, part).start()
        if shared and k == 0:
            @pl.when(group < groups - 1)
            def _():
                pl.semaphore_wait(here, groups - 1 - group)

            for other in range(1, groups):
                flag_copy(other).start()

    if opening:
        gate_own = column(row == col, gate_row(0))
        gate_near = column(row == col, gate_row(1))
        near_copy().wait_recv()
        hidden = hidden_of(both[...])
        for cols in blocks:
            result = dot(hidden, wd[:, cols])
            total[:, cols] = result[:tok_count] * gate_own
            near_res[:, cols] = (result[tok_count:] * gate_near).astype(BF16)
        near_return().start()

    place_col = column(row == col, place).astype(jnp.int32)

    def spread(at, count):
        want = start + at + lax.broadcasted_iota(jnp.int32, (tok_count, count), 1)
        return jnp.where(place_col == want, 1.0, 0.0).astype(BF16)

    if opening:
        near_return().wait_recv()
        total[...] = total[...] + near_back[...].astype(F32)
    else:
        total[...] = base_ref[...].astype(F32)
    if shared:
        received(flag_in.at[pl.ds(1, groups - 1)], flag_recv.at[0])
        flag = flag_out[...]
        for k in range(1, groups):
            flag = jnp.maximum(flag, flag_in[k])
        flag_ref[0, 0] = jnp.max(flag).astype(jnp.int32)
    if steps > 1:
        received(far_back.at[pl.ds(0, starts[-1])], back_recv.at[0])
        total[...] = total[...] + dot(spread(0, starts[-1]), far_back[pl.ds(0, starts[-1]), :])
    last = spread(starts[-1], sizes[-1])
    for part, cols in enumerate(halves):
        far_return(steps - 1, part).wait_recv()
        out_ref[:, cols] = (total[:, cols] + dot(last, far_back[span(steps - 1), cols])).astype(BF16)

    for i in (0, 4, 5, 6):
        sent(far_out, i)
    for i in range(2):
        sent((ids_all, gates_all)[i].at[pl.ds(1, tp_count - 1)], 1 + i)
    if opening:
        sent(both, 3)
    if shared:
        sent(flag_in.at[pl.ds(1, groups - 1)], 7)


def pair_call(tp_count, cores, start, sizes, shared, arrays, base=None):
    tok_count, width = arrays[0].shape
    hidden = arrays[5].shape[2]
    opening = base is None
    cap = sum(sizes)
    groups = lax.axis_size("ep") * lax.axis_size("grp")
    whole = pltpu.VMEM((tok_count, width), BF16)
    part = pltpu.VMEM((cap, width), BF16)
    dma = pltpu.SemaphoreType.DMA
    scratch = [
        whole,
        pltpu.VMEM((2, 1, width), F32),
        pltpu.VMEM((tp_count, 2, tok_count), jnp.int32),
        pltpu.VMEM((tp_count, 2, tok_count), F32),
        pltpu.VMEM((2, width, hidden), BF16),
        pltpu.VMEM((hidden, width), BF16),
        pltpu.VMEM((2 * tok_count, width), BF16),
        pltpu.VMEM((tok_count, width), F32),
        whole,
        part,
        pltpu.VMEM((sizes[0], width), BF16),
        pltpu.VMEM((2 * cap, width), BF16),
        pltpu.VMEM((max(sizes), width), F32),
        part, part, part, part,
        dma((8,)), dma((len(sizes),)), dma((2, 2)), dma((1 + pl.cdiv(width, TAIL_COLS),)), dma((2,)),
    ]
    if opening:
        scratch += [whole, dma((2,))]
    if shared:
        scratch += [
            pltpu.VMEM((8, 128), F32), pltpu.VMEM((groups, 8, 128), F32), dma((1,)), pltpu.SemaphoreType.REGULAR,
        ]
    out_shape = [pltpu.VMEM((tok_count, width), BF16)]
    out_specs = [pl.BlockSpec(memory_space=pltpu.VMEM)]
    if shared:
        out_shape.append(pltpu.SMEM((1, 1), jnp.int32))
        out_specs.append(pl.BlockSpec(memory_space=pltpu.SMEM))
    in_specs = [pl.BlockSpec(memory_space=IN_SPACE)] * len(arrays)
    arrays = [pltpu.with_memory_space_constraint(x, pltpu.HBM) for x in arrays]
    if not opening:
        arrays.append(base)
        in_specs.append(pl.BlockSpec(memory_space=pltpu.VMEM))
    return pl.pallas_call(
        functools.partial(pair_kernel, tp_count, cores, start, sizes, opening, shared),
        out_shape=out_shape,
        in_specs=in_specs,
        out_specs=out_specs,
        scratch_shapes=scratch,
        compiler_params=pltpu.CompilerParams(
            collective_id=0 if opening else 1, has_side_effects=True, vmem_limit_bytes=VMEM_BYTES
        ),
    )(*arrays)


def cut(rows):
    return [min(STEP_ROWS, rows - at) for at in range(0, rows, STEP_ROWS)]


def pair_shards(tp_count, cores, arrays):
    tok_count = arrays[0].shape[0]
    cap = tok_count - (tok_count // KEEP if KEEP else 0)
    if cap == tok_count:
        return pair_call(tp_count, cores, 0, cut(cap), False, arrays)[0]
    out, flag = pair_call(tp_count, cores, 0, cut(cap), True, arrays)
    return lax.cond(
        flag[0, 0] > 0,
        lambda: pair_call(tp_count, cores, cap, cut(tok_count - cap), False, arrays, out)[0],
        lambda: out,
    )


def shards(token_rows, norm_gain, norm_bias, expert_ids, route_gates, gate_weight, up_weight, down_weight):
    tok_count, width = token_rows.shape
    hidden = gate_weight.shape[2]
    tp_count = lax.axis_size("tp")
    capacity = min(4 * tok_count // tp_count, tok_count // 2)
    cores = 2
    arrays = [
        token_rows, norm_gain.reshape(1, width), norm_bias.reshape(1, width),
        expert_ids.T, route_gates.T, gate_weight, up_weight, down_weight,
    ]
    if tp_count == 2 * cores:
        return pair_shards(tp_count, cores, arrays)
    far = tp_count - cores
    chunks = max(1, capacity // CHUNK_ROWS)
    rows = capacity // chunks
    near = pltpu.VMEM((cores, capacity, width), BF16)
    distant = pltpu.VMEM((chunks, far, rows, width), BF16)
    near_sem = pltpu.SemaphoreType.DMA((cores,))
    far_sem = pltpu.SemaphoreType.DMA((chunks, far))
    ret_sem = pltpu.SemaphoreType.DMA((chunks, far, BLOCKS))
    return pl.pallas_call(
        functools.partial(kernel, tp_count, cores, capacity, chunks),
        out_shape=pltpu.VMEM((tok_count, width), BF16),
        in_specs=[pl.BlockSpec(memory_space=IN_SPACE)] * 8,
        out_specs=pl.BlockSpec(memory_space=pltpu.VMEM),
        scratch_shapes=[
            pltpu.VMEM((tok_count, width), BF16),
            pltpu.VMEM((1, width), F32),
            pltpu.VMEM((1, width), F32),
            pltpu.VMEM((2, tok_count), jnp.int32),
            pltpu.VMEM((2, tok_count), F32),
            pltpu.VMEM((width, hidden), BF16),
            pltpu.VMEM((width, hidden), BF16),
            pltpu.VMEM((hidden, width), BF16),
            pltpu.VMEM((max(cores * capacity, far * rows), width), BF16),
            near, near, near, near,
            distant, distant, distant, distant,
            pltpu.VMEM((tok_count, width), F32),
            pltpu.SemaphoreType.DMA((8,)),
            near_sem, near_sem, near_sem, near_sem,
            far_sem, far_sem, ret_sem, ret_sem,
        ],
        compiler_params=pltpu.CompilerParams(
            collective_id=0, has_side_effects=True, vmem_limit_bytes=VMEM_BYTES
        ),
    )(*(pltpu.with_memory_space_constraint(x, pltpu.HBM) for x in arrays))


def solution(mesh):
    rows = P(("grp", "ep", "tp"), None)
    weight = P("tp", None, None)
    return jax.shard_map(
        shards, mesh=mesh,
        in_specs=(rows, P(), P(), rows, rows, weight, weight, weight),
        out_specs=rows, check_vma=False,
    )
```
